32 devices in a mesh: sp: 4 (over z), tp: 4 (over y, x), dp: 2 (over core).
Axes of the slice: x: 2, y: 2, z: 4, core: 2. Of those that a mesh axis runs over, the one named last changes fastest.
Arguments:
- latent: bfloat16 [2, 1024, 2048], P('dp', 'sp'), may hold values from -1.5 to 1.5
- condition: bfloat16 [2, 2048], P('dp', 'sp'), may hold values from -6 to 6
- context: bfloat16 [2, 1024, 2048], P('dp', 'sp'), may hold values from -6 to 6
- context_code: bfloat16 [2048], P('sp'), may hold values from -6 to 6
- shift_weight: bfloat16 [2048, 2048], P('sp', 'tp'), may hold values from -0.125 to 0.125
- scale_weight: bfloat16 [2048, 2048], P('sp', 'tp'), may hold values from -0.125 to 0.125
- gate_weight: bfloat16 [2048, 2048], P('sp', 'tp'), may hold values from -0.125 to 0.125
- norm_gain: float32 [2048], replicated, may hold values from 0.1 to 1.9
- query_weight: bfloat16 [2048, 1024], P(None, 'tp'), may hold values from -0.125 to 0.125
- key_weight: bfloat16 [2048, 256], P(None, 'tp'), may hold values from -0.125 to 0.125
- value_weight: bfloat16 [2048, 256], P(None, 'tp'), may hold values from -0.125 to 0.125
- output_weight: bfloat16 [1024, 2048], P('tp'), may hold values from -0.75 to 0.75
- query_gain: float32 [64], replicated, may hold values from 1 to 5.5
- key_gain: float32 [64], replicated, may hold values from 1 to 5.5
- context_bias: float32 [16], P('tp'), may hold values from 0.5 to 2
Outputs:
- updated: bfloat16 [2, 1024, 2048], P('dp', 'sp')
The draws below stay inside these ranges and needn't reach their ends.
All inputs are finite; a program needn't handle non-finite values.
Results may differ from the reference program's by a relative error of at most 0.01405.
The reference program's roundings to bfloat16 on the way count: a program that leaves them out, or rounds other values in their place, can miss the bound.
Values may be sent and summed in bfloat16 or wider, within the bound.
A program may use at most 64 MiB of HBM per device.

```python
import math
import jax
import jax.numpy as jnp
from jax import lax

D = 2048
HEADS = 16
KV_HEADS = 4
HEAD = 64
GRID_W = 64
CTX = 1024
SAMPLES = 2
SEQ = 1024


def gain_draw(key, salt):
    fresh = jax.random.fold_in(key, salt)
    return jnp.exp(jax.random.uniform(fresh, (HEAD,), jnp.float32, 0.0, math.log(2.2)))


def draw_query_gain(key, part):
    return gain_draw(key, 17)


def draw_key_gain(key, part):
    return gain_draw(key, 29)


def shard_levels(rng, dims, cuts, smallest, largest):
    gain, own = 1.0, jax.random.fold_in(rng, 6)
    for dim, blocks in cuts:
        draws = jnp.exp(jax.random.uniform(jax.random.fold_in(own, dim), (blocks,), jnp.float32, smallest / len(cuts), largest / len(cuts)))
        gain = gain * jnp.repeat(draws, dims[dim] // blocks).reshape([-1 if axis == dim else 1 for axis in range(len(dims))])
    return gain


def centred(stream_key, dims, spread, bound, split=(), kind=jnp.bfloat16):
    entries = spread * jax.random.normal(stream_key, dims, jnp.float32)
    if split:
        entries = entries * shard_levels(stream_key, dims, split, -0.22, 0.18)
    return jnp.clip(entries, -bound, bound).astype(kind)


def setup_inputs(seed: int = 0) -> dict:
    key_of = jax.random.split(jax.random.key(seed), 16)
    latent = centred(key_of[0], (SAMPLES, SEQ, D), 0.25, 1.5, ((0, 2), (1, 4)))
    condition = centred(key_of[1], (SAMPLES, D), 1.0, 6.0, ((0, 2), (1, 4)))
    context = centred(key_of[2], (SAMPLES, CTX, D), 1.0, 6.0, ((0, 2), (1, 4)))
    context_code = centred(key_of[3], (D,), 1.0, 6.0, ((0, 4),))
    shift_weight = centred(key_of[4], (D, D), D ** -0.5, 0.125, ((0, 4), (1, 4)))
    scale_weight = centred(key_of[5], (D, D), D ** -0.5, 0.125, ((0, 4), (1, 4)))
    gate_weight = centred(key_of[6], (D, D), D ** -0.5, 0.125, ((0, 4), (1, 4)))
    norm_gain = jnp.clip(1.0 + 0.18 * jax.random.normal(key_of[7], (D,), jnp.float32), 0.1, 1.9)
    query_weight = centred(key_of[8], (D, HEADS * HEAD), D ** -0.5, 0.125, ((1, 4),))
    key_weight = centred(key_of[9], (D, KV_HEADS * HEAD), D ** -0.5, 0.125, ((1, 4),))
    value_weight = centred(key_of[10], (D, KV_HEADS * HEAD), D ** -0.5, 0.125, ((1, 4),))
    output_weight = centred(key_of[11], (HEADS * HEAD, D), (HEADS * HEAD // 16) ** -0.5, 0.75, ((0, 4),))
    query_gain = draw_query_gain(jax.random.fold_in(key_of[15], 71), 0)
    key_gain = draw_key_gain(jax.random.fold_in(key_of[15], 71), 0)
    context_bias = jnp.clip(0.5 + 1.5 * jax.random.uniform(key_of[14], (HEADS,), jnp.float32) ** shard_levels(key_of[14], (HEADS,), ((0, 4),), -0.2, 0.2), 0.5, 2.0)
    return {"latent": latent, "condition": condition, "context": context, "context_code": context_code, "shift_weight": shift_weight, "scale_weight": scale_weight, "gate_weight": gate_weight, "norm_gain": norm_gain, "query_weight": query_weight, "key_weight": key_weight, "value_weight": value_weight, "output_weight": output_weight, "query_gain": query_gain, "key_gain": key_gain, "context_bias": context_bias}


norm_eps = 1e-06
rope_base = 10000.0

def rotary_tables(position):
    grid_row = (position // GRID_W).astype(jnp.float32)
    grid_col = (position % GRID_W).astype(jnp.float32)
    quarter = HEAD // 4
    inverse = rope_base ** (-jnp.arange(quarter, dtype=jnp.float32) / quarter)
    angles = jnp.concatenate([grid_row[:, None] * inverse, grid_col[:, None] * inverse], axis=-1)
    return (jnp.cos(angles), jnp.sin(angles))

def head_norm(values, gain_row):
    return values * lax.rsqrt(lax.optimization_barrier(jnp.mean(values * values, axis=-1, keepdims=True)) + norm_eps) * gain_row

def rotate(values, cosine, sine_part):
    half_dim = values.shape[-1] // 2
    first_half = values[..., :half_dim]
    second_half = values[..., half_dim:]
    cos_rows = cosine[:, None, :]
    sin_rows = sine_part[:, None, :]
    return jnp.concatenate([first_half * cos_rows - second_half * sin_rows, second_half * cos_rows + first_half * sin_rows], axis=-1)

def modulated(tokens, gain_row, shift_row, scale_row):
    floats = tokens.astype(jnp.float32)
    normal = floats * lax.rsqrt(lax.optimization_barrier(jnp.mean(floats * floats, axis=-1, keepdims=True)) + norm_eps)
    return (normal * gain_row * (1.0 + scale_row) + shift_row).astype(jnp.bfloat16)

def attend(query_block, latent_keys, latent_values, context_keys, context_values, bias_value):
    score_scale = HEAD ** (-0.5)
    latent_scores = jnp.dot(query_block, latent_keys.T, preferred_element_type=jnp.float32) * score_scale
    context_scores = jnp.dot(query_block, context_keys.T, preferred_element_type=jnp.float32) * score_scale + bias_value
    row_max = jnp.maximum(latent_scores.max(axis=1), context_scores.max(axis=1))[:, None]
    latent_exp = jnp.exp(latent_scores - row_max)
    context_exp = jnp.exp(context_scores - row_max)
    totals = latent_exp.sum(axis=1) + context_exp.sum(axis=1)
    summed = jnp.dot(latent_exp.astype(jnp.bfloat16), latent_values, preferred_element_type=jnp.float32)
    summed = summed + jnp.dot(context_exp.astype(jnp.bfloat16), context_values, preferred_element_type=jnp.float32)
    return (summed / totals[:, None]).astype(jnp.bfloat16)

def reference(latent, condition, context, context_code, shift_weight, scale_weight, gate_weight, norm_gain, query_weight, key_weight, value_weight, output_weight, query_gain, key_gain, context_bias):
    cosine, sine_part = rotary_tables(jnp.arange(SEQ, dtype=jnp.int32))
    group_size = HEADS // KV_HEADS
    query_block = math.gcd(SEQ, 512)
    context_act = jax.nn.silu(context_code.astype(jnp.float32)).astype(jnp.bfloat16)
    context_shift = jnp.dot(context_act, shift_weight, preferred_element_type=jnp.float32)
    context_scale = jnp.dot(context_act, scale_weight, preferred_element_type=jnp.float32)
    results = []
    for sample in range(SAMPLES):
        activated = jax.nn.silu(condition[sample].astype(jnp.float32)).astype(jnp.bfloat16)
        latent_shift = jnp.dot(activated, shift_weight, preferred_element_type=jnp.float32)
        latent_scale = jnp.dot(activated, scale_weight, preferred_element_type=jnp.float32)
        latent_gate = jnp.dot(activated, gate_weight, preferred_element_type=jnp.float32)
        normed = modulated(latent[sample], norm_gain, latent_shift, latent_scale)
        queries = jnp.dot(normed, query_weight, preferred_element_type=jnp.float32).reshape(SEQ, HEADS, HEAD)
        queries = rotate(head_norm(queries, query_gain), cosine, sine_part).astype(jnp.bfloat16)
        latent_keys = jnp.dot(normed, key_weight, preferred_element_type=jnp.float32).reshape(SEQ, KV_HEADS, HEAD)
        latent_keys = rotate(head_norm(latent_keys, key_gain), cosine, sine_part).astype(jnp.bfloat16)
        latent_values = jnp.dot(normed, value_weight, preferred_element_type=jnp.float32)
        latent_values = latent_values.reshape(SEQ, KV_HEADS, HEAD).astype(jnp.bfloat16)
        context_normed = modulated(context[sample], norm_gain, context_shift, context_scale)
        context_keys = jnp.dot(context_normed, key_weight, preferred_element_type=jnp.float32).reshape(CTX, KV_HEADS, HEAD)
        context_keys = head_norm(context_keys, key_gain).astype(jnp.bfloat16)
        context_values = jnp.dot(context_normed, value_weight, preferred_element_type=jnp.float32)
        context_values = context_values.reshape(CTX, KV_HEADS, HEAD).astype(jnp.bfloat16)
        mixed = jnp.zeros((SEQ, D), jnp.float32)
        for kv_head in range(KV_HEADS):
            outputs = []
            for head_index in range(kv_head * group_size, (kv_head + 1) * group_size):
                head_out = lax.map(partial_attend(latent_keys[:, kv_head], latent_values[:, kv_head], context_keys[:, kv_head], context_values[:, kv_head], context_bias[head_index]), queries[:, head_index].reshape(SEQ // query_block, query_block, HEAD))
                outputs.append(head_out.reshape(SEQ, HEAD))
            attended = jnp.concatenate(outputs, axis=1)
            rows_start = kv_head * group_size * HEAD
            weight_rows = output_weight[rows_start:rows_start + group_size * HEAD]
            partial_sum = jnp.dot(attended, weight_rows, preferred_element_type=jnp.float32).astype(jnp.bfloat16)
            mixed = mixed + partial_sum.astype(jnp.float32)
        updated = latent[sample].astype(jnp.float32) + latent_gate * mixed
        results.append(updated.astype(jnp.bfloat16))
    return jnp.stack(results)

def partial_attend(latent_keys, latent_values, context_keys, context_values, bias_value):

    def attend_block(query_block):
        return attend(query_block, latent_keys, latent_values, context_keys, context_values, bias_value)
    return attend_block
```

```python
import functools
import math

import jax
import jax.numpy as jnp
from jax import lax
from jax.experimental import pallas as pl
from jax.experimental.pallas import tpu as pltpu
from jax.sharding import PartitionSpec as P

GRID_W = 64
norm_eps = 1e-06
rope_base = 10000.0
F32 = jnp.float32
BF16 = jnp.bfloat16
LOW = -1e30


def tables(first, rows, head_dim):
    quarter = head_dim // 4
    half = head_dim // 2
    shape = (rows, head_dim)
    token = first + lax.broadcasted_iota(jnp.int32, shape, 0)
    lane = lax.broadcasted_iota(jnp.int32, shape, 1)
    pair = lane % half
    index = (pair % quarter).astype(F32)
    place = jnp.where(pair < quarter, token // GRID_W, token % GRID_W).astype(F32)
    angle = place * jnp.exp(index * (-math.log(rope_base) / quarter))
    sine = jnp.sin(angle)
    return jnp.cos(angle), jnp.where(lane < half, -sine, sine)


def head_norm(values, gain_row):
    mean = jnp.mean(values * values, axis=-1, keepdims=True)
    return values * lax.rsqrt(mean + norm_eps) * gain_row


def rotate(values, cosine, sine):
    half = values.shape[-1] // 2
    swapped = jnp.concatenate([values[:, half:], values[:, :half]], axis=1)
    return values * cosine + swapped * sine


def kernel(
    sizes,
    condition, code, gain_ref, q_gain, k_gain, bias_ref,
    latent, context, shift_w, scale_w, gate_w, wq, wk, wv, wo,
    out,
    modw, lat, ctx, wq_v, wkv, wbuf,
    vec_z, vec_t, normed, kvbuf, q_s, m_s, acc, att, mixed, cos_s, sin_s, inv_s, out_v,
    local, out_sem,
    z_send, z_recv, t_send, t_recv, kv_send, kv_recv,
    w_send, w_recv, f_send, f_recv, a_send, a_recv,
):
    n_sp, n_tp, n_dp = sizes
    sp, tp, dp = lax.axis_index("sp"), lax.axis_index("tp"), lax.axis_index("dp")
    rows, crows = lat.shape[0], ctx.shape[0]
    hd = wk.shape[0]
    qcols = wq_v.shape[1]
    heads = qcols // hd
    width = lat.shape[1]
    cols = width // n_tp
    dots = functools.partial(jnp.dot, preferred_element_type=F32)

    copies = {}
    for number, (name, src, dst) in enumerate((
        ("m0", shift_w, modw.at[0]), ("m1", scale_w, modw.at[1]), ("m2", gate_w, modw.at[2]),
        ("wk", wk, wkv.at[:hd]), ("wv", wv, wkv.at[hd:]), ("ctx", context.at[0], ctx), ("lat", latent.at[0], lat),
        ("wq", wq, wq_v), ("wo", wo, wbuf.at[tp]),
    )):
        copies[name] = pltpu.make_async_copy(src, dst, local.at[number])
        copies[name].start()

    barrier = pltpu.get_barrier_semaphore()
    for d in range(1, n_sp):
        pl.semaphore_signal(barrier, inc=1, device_id={"sp": (sp + d) % n_sp}, device_id_type=pl.DeviceIdType.MESH)
    for d in range(1, n_tp):
        pl.semaphore_signal(barrier, inc=1, device_id={"tp": tp ^ d}, device_id_type=pl.DeviceIdType.MESH)
    for d in range(1, n_dp):
        pl.semaphore_signal(barrier, inc=1, device_id={"dp": (dp + d) % n_dp}, device_id_type=pl.DeviceIdType.MESH)

    def remote(src, dst, s, r, **where):
        return pltpu.make_async_remote_copy(
            src_ref=src, dst_ref=dst, send_sem=s, recv_sem=r,
            device_id=where, device_id_type=pl.DeviceIdType.MESH)

    row8 = lax.broadcasted_iota(jnp.int32, (8, condition.shape[1]), 0)
    own_code = condition[...].astype(F32)
    shared_code = code[...].astype(F32)
    both = jnp.where(row8 == 0, own_code, jnp.where(row8 == 1, shared_code, 0.0))
    both = (both / (1.0 + jnp.exp(-both))).astype(BF16)
    pieces = []
    for k in range(3):
        copies[f"m{k}"].wait()
        pieces.append(dots(both, modw[k])[:2])
    vec_z[sp] = jnp.concatenate(pieces + [jnp.zeros_like(pieces[0])], axis=0)

    pl.semaphore_wait(barrier, n_sp + n_tp + n_dp - 3)
    z_copies = []
    for d in range(1, n_sp):
        copy = remote(vec_z.at[sp], vec_z.at[sp], z_send.at[d], z_recv.at[d], sp=(sp + d) % n_sp)
        copy.start()
        z_copies.append(copy)

    share = wo.shape[0] // n_dp
    piece = share // 2

    def span(core, part):
        return pl.ds(core * share + part * piece, piece)

    near = [d for d in (1, 2) if d < n_tp]
    waiting = []

    def send_weights(part):
        for d in near:
            copy = remote(wo.at[span(dp, part)], wbuf.at[tp, span(dp, part)],
                          w_send.at[d, part], w_recv.at[d, part], tp=tp ^ d)
            copy.start()
            waiting.append(copy)

    def got_weights(d, part):
        ref = wbuf.at[tp ^ d, span(dp, part)]
        remote(ref, ref, w_send.at[d, part], w_recv.at[d, part], tp=tp ^ d).wait_recv()
        if n_tp == 4 and (d, part) in ((2, 0), (1, 1)):
            copy = remote(ref, ref, w_send.at[3, part], w_recv.at[3, part], tp=tp ^ (3 - d))
            copy.start()
            waiting.append(copy)
        for e in range(1, n_dp):
            copy = remote(ref, ref, f_send.at[d, part, e], f_recv.at[d, part, e], dp=(dp + e) % n_dp)
            copy.start()
            waiting.append(copy)

    send_weights(0)

    cosine, sine = tables(sp * rows, rows, hd)
    cos_s[...] = cosine
    sin_s[...] = sine
    copies["ctx"].wait()
    floats = ctx[...].astype(F32)
    inv_c = lax.rsqrt(jnp.mean(floats * floats, axis=-1, keepdims=True) + norm_eps)
    copies["lat"].wait()
    floats = lat[...].astype(F32)
    inv_s[...] = lax.rsqrt(jnp.mean(floats * floats, axis=-1, keepdims=True) + norm_eps)

    for copy in z_copies:
        copy.wait()
    total = vec_z[0]
    for k in range(1, n_sp):
        total = total + vec_z[k]
    vec_t[tp] = total
    for d in range(1, n_tp):
        copy = remote(vec_t.at[tp], vec_t.at[tp], t_send.at[d], t_recv.at[d], tp=tp ^ d)
        copy.start()
        waiting.append(copy)
    send_weights(1)
    for d in range(1, n_tp):
        remote(vec_t.at[tp ^ d], vec_t.at[tp ^ d], t_send.at[d], t_recv.at[d], tp=tp ^ d).wait_recv()

    def modulate(tokens, inverse, which):
        for t in range(n_tp):
            part = slice(t * cols, (t + 1) * cols)
            factor = gain_ref[:, part] * (1.0 + vec_t[t, 2 + which:3 + which, :])
            shift = vec_t[t, which:which + 1, :]
            normed[:tokens.shape[0], part] = (tokens[:, part].astype(F32) * inverse * factor + shift).astype(BF16)

    lanes = 2 * hd

    def kv_copy(block, target, way, part):
        area = pl.ds(0, crows) if part == 0 else pl.ds(crows, rows)
        ref = kvbuf.at[block, area]
        return remote(ref, ref, kv_send.at[way, part, block], kv_recv.at[part, block], sp=target)

    def send_own(part):
        @pl.when(sp + 1 < n_sp)
        def _():
            kv_copy(sp, sp + 1, 0, part).start()

        @pl.when(sp > 0)
        def _():
            kv_copy(sp, sp - 1, 1, part).start()

    dims = (((1,), (1,)), ((), ()))
    modulate(ctx, inv_c, 1)
    copies["wk"].wait()
    copies["wv"].wait()
    kv = lax.dot_general(normed[:crows], wkv[...], dims, preferred_element_type=F32)
    kvbuf[sp, :crows] = jnp.concatenate([head_norm(kv[:, :hd], k_gain[...]), kv[:, hd:]], axis=1).astype(BF16)
    send_own(0)

    modulate(lat, inv_s[...], 0)
    kv = lax.dot_general(normed[:rows], wkv[...], dims, preferred_element_type=F32)
    keys = rotate(head_norm(kv[:, :hd], k_gain[...]), cos_s[...], sin_s[...])
    kvbuf[sp, crows:] = jnp.concatenate([keys, kv[:, hd:]], axis=1).astype(BF16)
    send_own(1)

    copies["wq"].wait()
    queries = dots(normed[:rows], wq_v[...])
    for h in range(heads):
        one = rotate(head_norm(queries[:, h * hd:(h + 1) * hd], q_gain[...]), cos_s[...], sin_s[...])
        q_s[h] = (one * hd ** -0.5).astype(BF16)
    m_s[...] = jnp.full_like(m_s, LOW)
    acc[...] = jnp.zeros_like(acc)

    for d in near:
        got_weights(d, 0)

    def absorb(block):
        @pl.loop(0, heads)
        def _(h):
            bias = bias_ref[h]
            query = q_s[h]
            s_c = lax.dot_general(query, kvbuf[block, :crows, :hd], dims, preferred_element_type=F32)
            s_l = lax.dot_general(query, kvbuf[block, crows:, :hd], dims, preferred_element_type=F32)
            old = m_s[h]
            new = jnp.maximum(old, jnp.maximum(
                s_c.max(axis=1, keepdims=True) + bias, s_l.max(axis=1, keepdims=True)))
            m_s[h] = new
            p_c = jnp.exp(s_c - (new - bias)).astype(BF16)
            p_l = jnp.exp(s_l - new).astype(BF16)

            def values(pairs):
                lane = lax.broadcasted_iota(jnp.int32, pairs.shape, 1)
                return jnp.where(lane < hd, jnp.ones_like(pairs), pairs)

            acc[h] = (acc[h] * jnp.exp(old - new)
                      + dots(p_c, values(kvbuf[block, :crows]))
                      + dots(p_l, values(kvbuf[block, crows:])))

    absorb(sp)
    for d in near:
        got_weights(d, 1)

    @pl.loop(1, n_sp)
    def _(s):
        for part in range(2):
            @pl.when(sp - s >= 0)
            def _():
                kv_copy(sp - s, sp, 0, part).wait_recv()

                @pl.when(sp + 1 < n_sp)
                def _():
                    kv_copy(sp - s, sp + 1, 0, part).start()

            @pl.when(sp + s < n_sp)
            def _():
                kv_copy(sp + s, sp, 1, part).wait_recv()

                @pl.when(sp > 0)
                def _():
                    kv_copy(sp + s, sp - 1, 1, part).start()

        @pl.when(sp - s >= 0)
        def _():
            absorb(sp - s)

        @pl.when(sp + s < n_sp)
        def _():
            absorb(sp + s)

    if n_tp == 4:
        for part in range(2):
            got_weights(3, part)

    for g in range(heads // 2):
        pair = []
        for h in (2 * g, 2 * g + 1):
            whole = acc[h]
            pair.append(whole[:, hd:] / whole[:, :hd])
        att[tp, g] = jnp.concatenate(pair, axis=1).astype(BF16)
        for d in range(1, n_tp):
            copy = remote(att.at[tp, g], att.at[tp, g], a_send.at[d, g], a_recv.at[d, g], tp=tp ^ d)
            copy.start()
            waiting.append(copy)

    copies["wo"].wait()
    step = cols

    def project(group):
        left = jnp.concatenate([att[group, g] for g in range(heads // 2)], axis=1)
        return lambda part: dots(left, wbuf[group, :, part]).astype(BF16).astype(F32)

    def arrive(d):
        for core in range(1, n_dp):
            source = (dp + n_dp - core) % n_dp
            for part in range(2):
                ref = wbuf.at[tp ^ d, span(source, part)]
                remote(ref, ref, f_send.at[d, part, core], f_recv.at[d, part, core], dp=source).wait_recv()
        for g in range(heads // 2):
            ref = att.at[tp ^ d, g]
            remote(ref, ref, a_send.at[d, g], a_recv.at[d, g], tp=tp ^ d).wait_recv()
        return project(tp ^ d)

    for d in range(n_tp):
        term = project(tp) if d == 0 else arrive(d)
        for t in range(n_tp):
            part = slice(t * step, (t + 1) * step)
            value = term(part)
            if d > 0:
                value = mixed[:, part] + value
            if d < n_tp - 1:
                mixed[:, part] = value
            else:
                gate = vec_t[t, 4:5, :]
                out_v[:, part] = (lat[:, part].astype(F32) + gate * value).astype(BF16)
    back = pltpu.make_async_copy(out_v, out.at[0], out_sem)
    back.start()

    for copy in waiting:
        copy.wait_send()

    @pl.loop(0, n_sp)
    def _(b):
        for part in range(2):
            @pl.when((b <= sp) & (sp + 1 < n_sp))
            def _():
                kv_copy(b, sp, 0, part).wait_send()

            @pl.when((b >= sp) & (sp > 0))
            def _():
                kv_copy(b, sp, 1, part).wait_send()
    back.wait()


def on_device(
    sizes, latent, condition, context, context_code, shift_weight, scale_weight, gate_weight,
    norm_gain, query_weight, key_weight, value_weight, output_weight, query_gain, key_gain,
    context_bias,
):
    n_sp, n_tp, n_dp = sizes
    rows, width = latent.shape[1:]
    crows = context.shape[1]
    hd = query_gain.shape[0]
    qcols = query_weight.shape[1]
    heads = qcols // hd
    deep, cols = shift_weight.shape
    vmem = pl.BlockSpec(memory_space=pltpu.VMEM)
    smem = pl.BlockSpec(memory_space=pltpu.SMEM)
    hbm = pl.BlockSpec(memory_space=pl.ANY)
    dma = pltpu.SemaphoreType.DMA
    most = max(rows, crows)
    scratch = [
        pltpu.VMEM((3, deep, cols), BF16),
        pltpu.VMEM((rows, width), BF16),
        pltpu.VMEM((crows, width), BF16),
        pltpu.VMEM((width, qcols), BF16),
        pltpu.VMEM((2 * hd, width), BF16),
        pltpu.VMEM((n_tp,) + output_weight.shape, BF16),
        pltpu.VMEM((n_sp, 8, cols), F32),
        pltpu.VMEM((n_tp, 8, cols), F32),
        pltpu.VMEM((most, width), BF16),
        pltpu.VMEM((n_sp, crows + rows, 2 * hd), BF16),
        pltpu.VMEM((heads, rows, hd), BF16),
        pltpu.VMEM((heads, rows, 1), F32),
        pltpu.VMEM((heads, rows, 2 * hd), F32),
        pltpu.VMEM((n_tp, heads // 2, rows, 2 * hd), BF16),
        pltpu.VMEM((rows, width), F32),
        pltpu.VMEM((rows, hd), F32),
        pltpu.VMEM((rows, hd), F32),
        pltpu.VMEM((rows, 1), F32),
        pltpu.VMEM((rows, width), BF16),
        dma((9,)), dma,
        dma((n_sp,)), dma((n_sp,)), dma((n_tp,)), dma((n_tp,)),
        dma((2, 2, n_sp)), dma((2, n_sp)),
        dma((n_tp, 2)), dma((n_tp, 2)), dma((n_tp, 2, n_dp)), dma((n_tp, 2, n_dp)),
        dma((n_tp, heads // 2)), dma((n_tp, heads // 2)),
    ]
    return pl.pallas_call(
        functools.partial(kernel, sizes),
        out_shape=jax.ShapeDtypeStruct(latent.shape, BF16),
        in_specs=[vmem] * 5 + [smem] + [hbm] * 9,
        out_specs=hbm,
        scratch_shapes=scratch,
        compiler_params=pltpu.CompilerParams(
            collective_id=0, has_side_effects=True, vmem_limit_bytes=60 * 1024 * 1024),
    )(
        condition, context_code[None], norm_gain[None], query_gain[None], key_gain[None],
        context_bias, latent, context, shift_weight, scale_weight, gate_weight, query_weight,
        key_weight.T, value_weight.T, output_weight,
    )


def solution(mesh):
    sizes = tuple(mesh.shape[axis] for axis in ("sp", "tp", "dp"))
    return jax.shard_map(
        functools.partial(on_device, sizes),
        mesh=mesh,
        in_specs=(
            P("dp", "sp", None),
            P("dp", "sp"),
            P("dp", "sp", None),
            P("sp"),
            P("sp", "tp"),
            P("sp", "tp"),
            P("sp", "tp"),
            P(),
            P(None, "tp"),
            P(None, "tp"),
            P(None, "tp"),
            P("tp", None),
            P(),
            P(),
            P("tp"),
        ),
        out_specs=P("dp", "sp", None),
        check_vma=False,
    )
```

```python
import functools
import math

import jax
import jax.numpy as jnp
from jax import lax
from jax.experimental import pallas as pl
from jax.experimental.pallas import tpu as pltpu
from jax.sharding import PartitionSpec as P

GRID_W = 64
norm_eps = 1e-06
rope_base = 10000.0
F32 = jnp.float32
BF16 = jnp.bfloat16
LOW = -1e30


def tables(first, rows, head_dim):
    quarter = head_dim // 4
    half = head_dim // 2
    shape = (rows, head_dim)
    token = first + lax.broadcasted_iota(jnp.int32, shape, 0)
    lane = lax.broadcasted_iota(jnp.int32, shape, 1)
    pair = lane % half
    index = (pair % quarter).astype(F32)
    place = jnp.where(pair < quarter, token // GRID_W, token % GRID_W).astype(F32)
    angle = place * jnp.exp(index * (-math.log(rope_base) / quarter))
    sine = jnp.sin(angle)
    return jnp.cos(angle), jnp.where(lane < half, -sine, sine)


def head_norm(values, gain_row):
    mean = jnp.mean(values * values, axis=-1, keepdims=True)
    return values * lax.rsqrt(mean + norm_eps) * gain_row


def rotate(values, cosine, sine):
    half = values.shape[-1] // 2
    swapped = jnp.concatenate([values[:, half:], values[:, :half]], axis=1)
    return values * cosine + swapped * sine


def kernel(
    sizes,
    condition, code, gain_ref, q_gain, k_gain, bias_ref,
    latent, context, shift_w, scale_w, gate_w, wq, wk, wv, wo,
    out,
    modw, lat, ctx, wq_v, wkv, wbuf,
    vec_z, vec_t, normed, kvbuf, q_s, m_s, acc, att, mixed, cos_s, sin_s, inv_s,
    local,
    z_send, z_recv, t_send, t_recv, kv_send, kv_recv,
    w_send, w_recv, f_send, f_recv, a_send, a_recv,
):
    n_sp, n_tp, n_dp = sizes
    sp, tp, dp = lax.axis_index("sp"), lax.axis_index("tp"), lax.axis_index("dp")
    rows, crows = lat.shape[0], ctx.shape[0]
    hd = wk.shape[0]
    qcols = wq_v.shape[1]
    heads = qcols // hd
    width = lat.shape[1]
    cols = width // n_tp
    dots = functools.partial(jnp.dot, preferred_element_type=F32)

    copies = {}
    for number, (name, src, dst) in enumerate((
        ("m0", shift_w, modw.at[0]), ("m1", scale_w, modw.at[1]), ("m2", gate_w, modw.at[2]),
        ("wk", wk, wkv.at[:hd]), ("wv", wv, wkv.at[hd:]), ("ctx", context.at[0], ctx), ("lat", latent.at[0], lat),
        ("wq", wq, wq_v), ("wo", wo, wbuf.at[tp]),
    )):
        copies[name] = pltpu.make_async_copy(src, dst, local.at[number])
        copies[name].start()

    barrier = pltpu.get_barrier_semaphore()
    for d in range(1, n_sp):
        pl.semaphore_signal(barrier, inc=1, device_id={"sp": (sp + d) % n_sp}, device_id_type=pl.DeviceIdType.MESH)
    for d in range(1, n_tp):
        pl.semaphore_signal(barrier, inc=1, device_id={"tp": tp ^ d}, device_id_type=pl.DeviceIdType.MESH)
    for d in range(1, n_dp):
        pl.semaphore_signal(barrier, inc=1, device_id={"dp": (dp + d) % n_dp}, device_id_type=pl.DeviceIdType.MESH)

    def remote(src, dst, s, r, **where):
        return pltpu.make_async_remote_copy(
            src_ref=src, dst_ref=dst, send_sem=s, recv_sem=r,
            device_id=where, device_id_type=pl.DeviceIdType.MESH)

    row8 = lax.broadcasted_iota(jnp.int32, (8, condition.shape[1]), 0)
    own_code = condition[...].astype(F32)
    shared_code = code[...].astype(F32)[None]
    both = jnp.where(row8 == 0, own_code, jnp.where(row8 == 1, shared_code, 0.0))
    both = (both / (1.0 + jnp.exp(-both))).astype(BF16)
    pieces = []
    for k in range(3):
        copies[f"m{k}"].wait()
        pieces.append(dots(both, modw[k])[:2])
    vec_z[sp] = jnp.concatenate(pieces + [jnp.zeros_like(pieces[0])], axis=0)

    pl.semaphore_wait(barrier, n_sp + n_tp + n_dp - 3)
    z_copies = []
    for d in range(1, n_sp):
        copy = remote(vec_z.at[sp], vec_z.at[sp], z_send.at[d], z_recv.at[d], sp=(sp + d) % n_sp)
        copy.start()
        z_copies.append(copy)

    share = wo.shape[0] // n_dp
    piece = share // 2

    def span(core, part):
        return pl.ds(core * share + part * piece, piece)

    near = [d for d in (1, 2) if d < n_tp]
    waiting = []

    def send_weights(part):
        for d in near:
            copy = remote(wo.at[span(dp, part)], wbuf.at[tp, span(dp, part)],
                          w_send.at[d, part], w_recv.at[d, part], tp=tp ^ d)
            copy.start()
            waiting.append(copy)

    def got_weights(d, part):
        ref = wbuf.at[tp ^ d, span(dp, part)]
        remote(ref, ref, w_send.at[d, part], w_recv.at[d, part], tp=tp ^ d).wait_recv()
        if n_tp == 4 and (d, part) in ((2, 0), (1, 1)):
            copy = remote(ref, ref, w_send.at[3, part], w_recv.at[3, part], tp=tp ^ (3 - d))
            copy.start()
            waiting.append(copy)
        for e in range(1, n_dp):
            copy = remote(ref, ref, f_send.at[d, part, e], f_recv.at[d, part, e], dp=(dp + e) % n_dp)
            copy.start()
            waiting.append(copy)

    send_weights(0)

    cosine, sine = tables(sp * rows, rows, hd)
    cos_s[...] = cosine
    sin_s[...] = sine
    copies["ctx"].wait()
    floats = ctx[...].astype(F32)
    inv_c = lax.rsqrt(jnp.mean(floats * floats, axis=-1, keepdims=True) + norm_eps)
    copies["lat"].wait()
    floats = lat[...].astype(F32)
    inv_s[...] = lax.rsqrt(jnp.mean(floats * floats, axis=-1, keepdims=True) + norm_eps)

    for copy in z_copies:
        copy.wait()
    total = vec_z[0]
    for k in range(1, n_sp):
        total = total + vec_z[k]
    vec_t[tp] = total
    for d in range(1, n_tp):
        copy = remote(vec_t.at[tp], vec_t.at[tp], t_send.at[d], t_recv.at[d], tp=tp ^ d)
        copy.start()
        waiting.append(copy)
    send_weights(1)
    for d in range(1, n_tp):
        remote(vec_t.at[tp ^ d], vec_t.at[tp ^ d], t_send.at[d], t_recv.at[d], tp=tp ^ d).wait_recv()

    def modulate(tokens, inverse, which):
        for t in range(n_tp):
            part = slice(t * cols, (t + 1) * cols)
            factor = gain_ref[:, part] * (1.0 + vec_t[t, 2 + which:3 + which, :])
            shift = vec_t[t, which:which + 1, :]
            normed[:tokens.shape[0], part] = (tokens[:, part].astype(F32) * inverse * factor + shift).astype(BF16)

    lanes = 2 * hd

    def kv_copy(block, target, way, part):
        area = pl.ds(0, crows) if part == 0 else pl.ds(crows, rows)
        ref = kvbuf.at[block, area]
        return remote(ref, ref, kv_send.at[way, part, block], kv_recv.at[part, block], sp=target)

    def send_own(part):
        @pl.when(sp + 1 < n_sp)
        def _():
            kv_copy(sp, sp + 1, 0, part).start()

        @pl.when(sp > 0)
        def _():
            kv_copy(sp, sp - 1, 1, part).start()

    dims = (((1,), (1,)), ((), ()))
    modulate(ctx, inv_c, 1)
    copies["wk"].wait()
    copies["wv"].wait()
    kv = lax.dot_general(normed[:crows], wkv[...], dims, preferred_element_type=F32)
    kvbuf[sp, :crows] = jnp.concatenate([head_norm(kv[:, :hd], k_gain[...]), kv[:, hd:]], axis=1).astype(BF16)
    send_own(0)

    modulate(lat, inv_s[...], 0)
    kv = lax.dot_general(normed[:rows], wkv[...], dims, preferred_element_type=F32)
    keys = rotate(head_norm(kv[:, :hd], k_gain[...]), cos_s[...], sin_s[...])
    kvbuf[sp, crows:] = jnp.concatenate([keys, kv[:, hd:]], axis=1).astype(BF16)
    send_own(1)

    copies["wq"].wait()
    queries = dots(normed[:rows], wq_v[...])
    for h in range(heads):
        one = rotate(head_norm(queries[:, h * hd:(h + 1) * hd], q_gain[...]), cos_s[...], sin_s[...])
        q_s[h] = (one * hd ** -0.5).astype(BF16)
    m_s[...] = jnp.full_like(m_s, LOW)
    acc[...] = jnp.zeros_like(acc)

    for d in near:
        got_weights(d, 0)

    def absorb(block):
        @pl.loop(0, heads)
        def _(h):
            bias = bias_ref[h]
            query = q_s[h]
            s_c = lax.dot_general(query, kvbuf[block, :crows, :hd], dims, preferred_element_type=F32)
            s_l = lax.dot_general(query, kvbuf[block, crows:, :hd], dims, preferred_element_type=F32)
            old = m_s[h]
            new = jnp.maximum(old, jnp.maximum(
                s_c.max(axis=1, keepdims=True) + bias, s_l.max(axis=1, keepdims=True)))
            m_s[h] = new
            p_c = jnp.exp(s_c - (new - bias)).astype(BF16)
            p_l = jnp.exp(s_l - new).astype(BF16)

            def values(pairs):
                lane = lax.broadcasted_iota(jnp.int32, pairs.shape, 1)
                return jnp.where(lane < hd, jnp.ones_like(pairs), pairs)

            acc[h] = (acc[h] * jnp.exp(old - new)
                      + dots(p_c, values(kvbuf[block, :crows]))
                      + dots(p_l, values(kvbuf[block, crows:])))

    absorb(sp)
    for d in near:
        got_weights(d, 1)

    @pl.loop(1, n_sp)
    def _(s):
        for part in range(2):
            @pl.when(sp - s >= 0)
            def _():
                kv_copy(sp - s, sp, 0, part).wait_recv()

                @pl.when(sp + 1 < n_sp)
                def _():
                    kv_copy(sp - s, sp + 1, 0, part).start()

            @pl.when(sp + s < n_sp)
            def _():
                kv_copy(sp + s, sp, 1, part).wait_recv()

                @pl.when(sp > 0)
                def _():
                    kv_copy(sp + s, sp - 1, 1, part).start()

        @pl.when(sp - s >= 0)
        def _():
            absorb(sp - s)

        @pl.when(sp + s < n_sp)
        def _():
            absorb(sp + s)

    if n_tp == 4:
        for part in range(2):
            got_weights(3, part)

    for g in range(heads // 2):
        pair = []
        for h in (2 * g, 2 * g + 1):
            whole = acc[h]
            pair.append(whole[:, hd:] / whole[:, :hd])
        att[tp, g] = jnp.concatenate(pair, axis=1).astype(BF16)
        for d in range(1, n_tp):
            copy = remote(att.at[tp, g], att.at[tp, g], a_send.at[d, g], a_recv.at[d, g], tp=tp ^ d)
            copy.start()
            waiting.append(copy)

    copies["wo"].wait()
    step = cols

    def project(group):
        left = jnp.concatenate([att[group, g] for g in range(heads // 2)], axis=1)
        return lambda part: dots(left, wbuf[group, :, part]).astype(BF16).astype(F32)

    def arrive(d):
        for core in range(1, n_dp):
            source = (dp + n_dp - core) % n_dp
            for part in range(2):
                ref = wbuf.at[tp ^ d, span(source, part)]
                remote(ref, ref, f_send.at[d, part, core], f_recv.at[d, part, core], dp=source).wait_recv()
        for g in range(heads // 2):
            ref = att.at[tp ^ d, g]
            remote(ref, ref, a_send.at[d, g], a_recv.at[d, g], tp=tp ^ d).wait_recv()
        return project(tp ^ d)

    for d in range(n_tp):
        term = project(tp) if d == 0 else arrive(d)
        for t in range(n_tp):
            part = slice(t * step, (t + 1) * step)
            value = term(part)
            if d > 0:
                value = mixed[:, part] + value
            if d < n_tp - 1:
                mixed[:, part] = value
            else:
                gate = vec_t[t, 4:5, :]
                out[0, :, part] = (lat[:, part].astype(F32) + gate * value).astype(BF16)

    for copy in waiting:
        copy.wait_send()

    @pl.loop(0, n_sp)
    def _(b):
        for part in range(2):
            @pl.when((b <= sp) & (sp + 1 < n_sp))
            def _():
                kv_copy(b, sp, 0, part).wait_send()

            @pl.when((b >= sp) & (sp > 0))
            def _():
                kv_copy(b, sp, 1, part).wait_send()


def on_device(
    sizes, latent, condition, context, context_code, shift_weight, scale_weight, gate_weight,
    norm_gain, query_weight, key_weight, value_weight, output_weight, query_gain, key_gain,
    context_bias,
):
    n_sp, n_tp, n_dp = sizes
    rows, width = latent.shape[1:]
    crows = context.shape[1]
    hd = query_gain.shape[0]
    qcols = query_weight.shape[1]
    heads = qcols // hd
    deep, cols = shift_weight.shape
    vmem = pl.BlockSpec(memory_space=pltpu.VMEM)
    smem = pl.BlockSpec(memory_space=pltpu.SMEM)
    hbm = pl.BlockSpec(memory_space=pltpu.HBM)
    dma = pltpu.SemaphoreType.DMA
    most = max(rows, crows)
    scratch = [
        pltpu.VMEM((3, deep, cols), BF16),
        pltpu.VMEM((rows, width), BF16),
        pltpu.VMEM((crows, width), BF16),
        pltpu.VMEM((width, qcols), BF16),
        pltpu.VMEM((2 * hd, width), BF16),
        pltpu.VMEM((n_tp,) + output_weight.shape, BF16),
        pltpu.VMEM((n_sp, 8, cols), F32),
        pltpu.VMEM((n_tp, 8, cols), F32),
        pltpu.VMEM((most, width), BF16),
        pltpu.VMEM((n_sp, crows + rows, 2 * hd), BF16),
        pltpu.VMEM((heads, rows, hd), BF16),
        pltpu.VMEM((heads, rows, 1), F32),
        pltpu.VMEM((heads, rows, 2 * hd), F32),
        pltpu.VMEM((n_tp, heads // 2, rows, 2 * hd), BF16),
        pltpu.VMEM((rows, width), F32),
        pltpu.VMEM((rows, hd), F32),
        pltpu.VMEM((rows, hd), F32),
        pltpu.VMEM((rows, 1), F32),
        dma((9,)),
        dma((n_sp,)), dma((n_sp,)), dma((n_tp,)), dma((n_tp,)),
        dma((2, 2, n_sp)), dma((2, n_sp)),
        dma((n_tp, 2)), dma((n_tp, 2)), dma((n_tp, 2, n_dp)), dma((n_tp, 2, n_dp)),
        dma((n_tp, heads // 2)), dma((n_tp, heads // 2)),
    ]
    return pl.pallas_call(
        functools.partial(kernel, sizes),
        out_shape=jax.ShapeDtypeStruct(latent.shape, BF16),
        in_specs=[vmem] * 5 + [smem] + [hbm] * 9,
        out_specs=vmem,
        scratch_shapes=scratch,
        compiler_params=pltpu.CompilerParams(
            collective_id=0, has_side_effects=True, vmem_limit_bytes=36 * 1024 * 1024),
    )(
        condition, context_code, norm_gain[None], query_gain[None], key_gain[None],
        context_bias, latent, context, shift_weight, scale_weight, gate_weight, query_weight,
        key_weight.T, value_weight.T, output_weight,
    )


def solution(mesh):
    sizes = tuple(mesh.shape[axis] for axis in ("sp", "tp", "dp"))
    return jax.shard_map(
        functools.partial(on_device, sizes),
        mesh=mesh,
        in_specs=(
            P("dp", "sp", None),
            P("dp", "sp"),
            P("dp", "sp", None),
            P("sp"),
            P("sp", "tp"),
            P("sp", "tp"),
            P("sp", "tp"),
            P(),
            P(None, "tp"),
            P(None, "tp"),
            P(None, "tp"),
            P("tp", None),
            P(),
            P(),
            P("tp"),
        ),
        out_specs=P("dp", "sp", None),
        check_vma=False,
    )
```

```python
import functools
import math

import jax
import jax.numpy as jnp
from jax import lax
from jax.experimental import pallas as pl
from jax.experimental.pallas import tpu as pltpu
from jax.sharding import PartitionSpec as P

GRID_W = 64
norm_eps = 1e-06
rope_base = 10000.0
F32 = jnp.float32
BF16 = jnp.bfloat16
LOW = -1e30


def tables(first, rows, head_dim):
    quarter = head_dim // 4
    half = head_dim // 2
    shape = (rows, head_dim)
    token = first + lax.broadcasted_iota(jnp.int32, shape, 0)
    lane = lax.broadcasted_iota(jnp.int32, shape, 1)
    pair = lane % half
    index = (pair % quarter).astype(F32)
    place = jnp.where(pair < quarter, token // GRID_W, token % GRID_W).astype(F32)
    angle = place * jnp.exp(index * (-math.log(rope_base) / quarter))
    sine = jnp.sin(angle)
    return jnp.cos(angle), jnp.where(lane < half, -sine, sine)


def head_norm(values, gain_row):
    mean = jnp.mean(values * values, axis=-1, keepdims=True)
    return values * lax.rsqrt(mean + norm_eps) * gain_row


def rotate(values, cosine, sine):
    half = values.shape[-1] // 2
    swapped = jnp.concatenate([values[:, half:], values[:, :half]], axis=1)
    return values * cosine + swapped * sine


def kernel(
    sizes,
    condition, code, gain_ref, q_gain, k_gain, bias_ref,
    latent, context, shift_w, scale_w, gate_w, wq, wk, wv, wo,
    out,
    modw, lat, ctx, wq_v, wkv, wbuf,
    vec_z, vec_t, normed, kvbuf, q_s, m_s, acc, att, mixed, cos_s, sin_s, inv_s, out_v,
    local, out_sem,
    z_send, z_recv, t_send, t_recv, kv_send, kv_recv,
    w_send, w_recv, f_send, f_recv, a_send, a_recv,
):
    n_sp, n_tp, n_dp = sizes
    sp, tp, dp = lax.axis_index("sp"), lax.axis_index("tp"), lax.axis_index("dp")
    rows, crows = lat.shape[0], ctx.shape[0]
    hd = wk.shape[0]
    qcols = wq_v.shape[1]
    heads = qcols // hd
    width = lat.shape[1]
    cols = width // n_tp
    dots = functools.partial(jnp.dot, preferred_element_type=F32)

    copies = {}
    for number, (name, src, dst) in enumerate((
        ("m0", shift_w, modw.at[0]), ("m1", scale_w, modw.at[1]), ("m2", gate_w, modw.at[2]),
        ("wk", wk, wkv.at[:hd]), ("wv", wv, wkv.at[hd:]), ("ctx", context.at[0], ctx), ("lat", latent.at[0], lat),
        ("wq", wq, wq_v), ("wo", wo, wbuf.at[tp]),
    )):
        copies[name] = pltpu.make_async_copy(src, dst, local.at[number])
        copies[name].start()

    barrier = pltpu.get_barrier_semaphore()
    for d in range(1, n_sp):
        pl.semaphore_signal(barrier, inc=1, device_id={"sp": (sp + d) % n_sp}, device_id_type=pl.DeviceIdType.MESH)
    for d in range(1, n_tp):
        pl.semaphore_signal(barrier, inc=1, device_id={"tp": tp ^ d}, device_id_type=pl.DeviceIdType.MESH)
    for d in range(1, n_dp):
        pl.semaphore_signal(barrier, inc=1, device_id={"dp": (dp + d) % n_dp}, device_id_type=pl.DeviceIdType.MESH)

    def remote(src, dst, s, r, **where):
        return pltpu.make_async_remote_copy(
            src_ref=src, dst_ref=dst, send_sem=s, recv_sem=r,
            device_id=where, device_id_type=pl.DeviceIdType.MESH)

    row8 = lax.broadcasted_iota(jnp.int32, (8, condition.shape[1]), 0)
    own_code = condition[...].astype(F32)
    shared_code = code[...].astype(F32)[None]
    both = jnp.where(row8 == 0, own_code, jnp.where(row8 == 1, shared_code, 0.0))
    both = (both / (1.0 + jnp.exp(-both))).astype(BF16)
    pieces = []
    for k in range(3):
        copies[f"m{k}"].wait()
        pieces.append(dots(both, modw[k])[:2])
    vec_z[sp] = jnp.concatenate(pieces + [jnp.zeros_like(pieces[0])], axis=0)

    pl.semaphore_wait(barrier, n_sp + n_tp + n_dp - 3)
    z_copies = []
    for d in range(1, n_sp):
        copy = remote(vec_z.at[sp], vec_z.at[sp], z_send.at[d], z_recv.at[d], sp=(sp + d) % n_sp)
        copy.start()
        z_copies.append(copy)

    share = wo.shape[0] // n_dp
    piece = share // 2

    def span(core, part):
        return pl.ds(core * share + part * piece, piece)

    near = [d for d in (1, 2) if d < n_tp]
    waiting = []

    def send_weights(part):
        for d in near:
            copy = remote(wo.at[span(dp, part)], wbuf.at[tp, span(dp, part)],
                          w_send.at[d, part], w_recv.at[d, part], tp=tp ^ d)
            copy.start()
            waiting.append(copy)

    def got_weights(d, part):
        ref = wbuf.at[tp ^ d, span(dp, part)]
        remote(ref, ref, w_send.at[d, part], w_recv.at[d, part], tp=tp ^ d).wait_recv()
        if n_tp == 4 and (d, part) in ((2, 0), (1, 1)):
            copy = remote(ref, ref, w_send.at[3, part], w_recv.at[3, part], tp=tp ^ (3 - d))
            copy.start()
            waiting.append(copy)
        for e in range(1, n_dp):
            copy = remote(ref, ref, f_send.at[d, part, e], f_recv.at[d, part, e], dp=(dp + e) % n_dp)
            copy.start()
            waiting.append(copy)

    send_weights(0)

    cosine, sine = tables(sp * rows, rows, hd)
    cos_s[...] = cosine
    sin_s[...] = sine
    copies["ctx"].wait()
    floats = ctx[...].astype(F32)
    inv_c = lax.rsqrt(jnp.mean(floats * floats, axis=-1, keepdims=True) + norm_eps)
    copies["lat"].wait()
    floats = lat[...].astype(F32)
    inv_s[...] = lax.rsqrt(jnp.mean(floats * floats, axis=-1, keepdims=True) + norm_eps)

    for copy in z_copies:
        copy.wait()
    total = vec_z[0]
    for k in range(1, n_sp):
        total = total + vec_z[k]
    vec_t[tp] = total
    for d in range(1, n_tp):
        copy = remote(vec_t.at[tp], vec_t.at[tp], t_send.at[d], t_recv.at[d], tp=tp ^ d)
        copy.start()
        waiting.append(copy)
    send_weights(1)
    for d in range(1, n_tp):
        remote(vec_t.at[tp ^ d], vec_t.at[tp ^ d], t_send.at[d], t_recv.at[d], tp=tp ^ d).wait_recv()

    def modulate(tokens, inverse, which):
        for t in range(n_tp):
            part = slice(t * cols, (t + 1) * cols)
            factor = gain_ref[:, part] * (1.0 + vec_t[t, 2 + which:3 + which, :])
            shift = vec_t[t, which:which + 1, :]
            normed[:tokens.shape[0], part] = (tokens[:, part].astype(F32) * inverse * factor + shift).astype(BF16)

    lanes = 2 * hd

    def kv_copy(block, target, way, part):
        area = pl.ds(0, crows) if part == 0 else pl.ds(crows, rows)
        ref = kvbuf.at[block, area]
        return remote(ref, ref, kv_send.at[way, part, block], kv_recv.at[part, block], sp=target)

    def send_own(part):
        @pl.when(sp + 1 < n_sp)
        def _():
            kv_copy(sp, sp + 1, 0, part).start()

        @pl.when(sp > 0)
        def _():
            kv_copy(sp, sp - 1, 1, part).start()

    dims = (((1,), (1,)), ((), ()))
    modulate(ctx, inv_c, 1)
    copies["wk"].wait()
    copies["wv"].wait()
    kv = lax.dot_general(normed[:crows], wkv[...], dims, preferred_element_type=F32)
    kvbuf[sp, :crows] = jnp.concatenate([head_norm(kv[:, :hd], k_gain[...]), kv[:, hd:]], axis=1).astype(BF16)
    send_own(0)

    modulate(lat, inv_s[...], 0)
    kv = lax.dot_general(normed[:rows], wkv[...], dims, preferred_element_type=F32)
    keys = rotate(head_norm(kv[:, :hd], k_gain[...]), cos_s[...], sin_s[...])
    kvbuf[sp, crows:] = jnp.concatenate([keys, kv[:, hd:]], axis=1).astype(BF16)
    send_own(1)

    copies["wq"].wait()
    queries = dots(normed[:rows], wq_v[...])
    for h in range(heads):
        one = rotate(head_norm(queries[:, h * hd:(h + 1) * hd], q_gain[...]), cos_s[...], sin_s[...])
        q_s[h] = (one * hd ** -0.5).astype(BF16)
    m_s[...] = jnp.full_like(m_s, LOW)
    acc[...] = jnp.zeros_like(acc)

    for d in near:
        got_weights(d, 0)

    def absorb(block):
        @pl.loop(0, heads)
        def _(h):
            bias = bias_ref[h]
            query = q_s[h]
            s_c = lax.dot_general(query, kvbuf[block, :crows, :hd], dims, preferred_element_type=F32)
            s_l = lax.dot_general(query, kvbuf[block, crows:, :hd], dims, preferred_element_type=F32)
            old = m_s[h]
            new = jnp.maximum(old, jnp.maximum(
                s_c.max(axis=1, keepdims=True) + bias, s_l.max(axis=1, keepdims=True)))
            m_s[h] = new
            p_c = jnp.exp(s_c - (new - bias)).astype(BF16)
            p_l = jnp.exp(s_l - new).astype(BF16)

            def values(pairs):
                lane = lax.broadcasted_iota(jnp.int32, pairs.shape, 1)
                return jnp.where(lane < hd, jnp.ones_like(pairs), pairs)

            acc[h] = (acc[h] * jnp.exp(old - new)
                      + dots(p_c, values(kvbuf[block, :crows]))
                      + dots(p_l, values(kvbuf[block, crows:])))

    absorb(sp)

    def forward(s):
        for part in range(2):
            @pl.when(sp - s >= 0)
            def _():
                kv_copy(sp - s, sp, 0, part).wait_recv()

                @pl.when(sp + 1 < n_sp)
                def _():
                    kv_copy(sp - s, sp + 1, 0, part).start()

            @pl.when(sp + s < n_sp)
            def _():
                kv_copy(sp + s, sp, 1, part).wait_recv()

                @pl.when(sp > 0)
                def _():
                    kv_copy(sp + s, sp - 1, 1, part).start()

    def absorb_both(s):
        @pl.when(sp - s >= 0)
        def _():
            absorb(sp - s)

        @pl.when(sp + s < n_sp)
        def _():
            absorb(sp + s)

    if n_sp > 1:
        forward(1)
    for d in near:
        got_weights(d, 1)
    if n_sp > 1:
        absorb_both(1)

    @pl.loop(2, n_sp)
    def _(s):
        forward(s)
        absorb_both(s)

    if n_tp == 4:
        for part in range(2):
            got_weights(3, part)

    for g in range(heads // 2):
        pair = []
        for h in (2 * g, 2 * g + 1):
            whole = acc[h]
            pair.append(whole[:, hd:] / whole[:, :hd])
        att[tp, g] = jnp.concatenate(pair, axis=1).astype(BF16)
        for d in range(1, n_tp):
            copy = remote(att.at[tp, g], att.at[tp, g], a_send.at[d, g], a_recv.at[d, g], tp=tp ^ d)
            copy.start()
            waiting.append(copy)

    copies["wo"].wait()
    step = cols

    def project(group):
        left = jnp.concatenate([att[group, g] for g in range(heads // 2)], axis=1)
        return lambda part: dots(left, wbuf[group, :, part]).astype(BF16).astype(F32)

    def arrive(d):
        for core in range(1, n_dp):
            source = (dp + n_dp - core) % n_dp
            for part in range(2):
                ref = wbuf.at[tp ^ d, span(source, part)]
                remote(ref, ref, f_send.at[d, part, core], f_recv.at[d, part, core], dp=source).wait_recv()
        for g in range(heads // 2):
            ref = att.at[tp ^ d, g]
            remote(ref, ref, a_send.at[d, g], a_recv.at[d, g], tp=tp ^ d).wait_recv()
        return project(tp ^ d)

    backs = []
    for d in range(n_tp):
        term = project(tp) if d == 0 else arrive(d)
        for t in range(n_tp):
            part = slice(t * step, (t + 1) * step)
            value = term(part)
            if d > 0:
                value = mixed[:, part] + value
            if d < n_tp - 1:
                mixed[:, part] = value
            else:
                gate = vec_t[t, 4:5, :]
                out_v[:, part] = (lat[:, part].astype(F32) + gate * value).astype(BF16)
                back = pltpu.make_async_copy(out_v.at[:, part], out.at[0, :, part], out_sem.at[t])
                back.start()
                backs.append(back)

    for copy in waiting:
        copy.wait_send()

    @pl.loop(0, n_sp)
    def _(b):
        for part in range(2):
            @pl.when((b <= sp) & (sp + 1 < n_sp))
            def _():
                kv_copy(b, sp, 0, part).wait_send()

            @pl.when((b >= sp) & (sp > 0))
            def _():
                kv_copy(b, sp, 1, part).wait_send()
    for back in backs:
        back.wait()


def on_device(
    sizes, latent, condition, context, context_code, shift_weight, scale_weight, gate_weight,
    norm_gain, query_weight, key_weight, value_weight, output_weight, query_gain, key_gain,
    context_bias,
):
    n_sp, n_tp, n_dp = sizes
    rows, width = latent.shape[1:]
    crows = context.shape[1]
    hd = query_gain.shape[0]
    qcols = query_weight.shape[1]
    heads = qcols // hd
    deep, cols = shift_weight.shape
    vmem = pl.BlockSpec(memory_space=pltpu.VMEM)
    smem = pl.BlockSpec(memory_space=pltpu.SMEM)
    hbm = pl.BlockSpec(memory_space=pl.ANY)
    dma = pltpu.SemaphoreType.DMA
    most = max(rows, crows)
    scratch = [
        pltpu.VMEM((3, deep, cols), BF16),
        pltpu.VMEM((rows, width), BF16),
        pltpu.VMEM((crows, width), BF16),
        pltpu.VMEM((width, qcols), BF16),
        pltpu.VMEM((2 * hd, width), BF16),
        pltpu.VMEM((n_tp,) + output_weight.shape, BF16),
        pltpu.VMEM((n_sp, 8, cols), F32),
        pltpu.VMEM((n_tp, 8, cols), F32),
        pltpu.VMEM((most, width), BF16),
        pltpu.VMEM((n_sp, crows + rows, 2 * hd), BF16),
        pltpu.VMEM((heads, rows, hd), BF16),
        pltpu.VMEM((heads, rows, 1), F32),
        pltpu.VMEM((heads, rows, 2 * hd), F32),
        pltpu.VMEM((n_tp, heads // 2, rows, 2 * hd), BF16),
        pltpu.VMEM((rows, width), F32),
        pltpu.VMEM((rows, hd), F32),
        pltpu.VMEM((rows, hd), F32),
        pltpu.VMEM((rows, 1), F32),
        pltpu.VMEM((rows, width), BF16),
        dma((9,)), dma((n_tp,)),
        dma((n_sp,)), dma((n_sp,)), dma((n_tp,)), dma((n_tp,)),
        dma((2, 2, n_sp)), dma((2, n_sp)),
        dma((n_tp, 2)), dma((n_tp, 2)), dma((n_tp, 2, n_dp)), dma((n_tp, 2, n_dp)),
        dma((n_tp, heads // 2)), dma((n_tp, heads // 2)),
    ]
    return pl.pallas_call(
        functools.partial(kernel, sizes),
        out_shape=jax.ShapeDtypeStruct(latent.shape, BF16),
        in_specs=[vmem] * 5 + [smem] + [hbm] * 9,
        out_specs=hbm,
        scratch_shapes=scratch,
        compiler_params=pltpu.CompilerParams(
            collective_id=0, has_side_effects=True, vmem_limit_bytes=60 * 1024 * 1024),
    )(
        condition, context_code, norm_gain[None], query_gain[None], key_gain[None],
        context_bias, latent, context, shift_weight, scale_weight, gate_weight, query_weight,
        key_weight.T, value_weight.T, output_weight,
    )


def solution(mesh):
    sizes = tuple(mesh.shape[axis] for axis in ("sp", "tp", "dp"))
    return jax.shard_map(
        functools.partial(on_device, sizes),
        mesh=mesh,
        in_specs=(
            P("dp", "sp", None),
            P("dp", "sp"),
            P("dp", "sp", None),
            P("sp"),
            P("sp", "tp"),
            P("sp", "tp"),
            P("sp", "tp"),
            P(),
            P(None, "tp"),
            P(None, "tp"),
            P(None, "tp"),
            P("tp", None),
            P(),
            P(),
            P("tp"),
        ),
        out_specs=P("dp", "sp", None),
        check_vma=False,
    )
```

```python
import functools
import math

import jax
import jax.numpy as jnp
from jax import lax
from jax.experimental import pallas as pl
from jax.experimental.pallas import tpu as pltpu
from jax.sharding import PartitionSpec as P

GRID_W = 64
norm_eps = 1e-06
rope_base = 10000.0
F32 = jnp.float32
BF16 = jnp.bfloat16
LOW = -1e30


def tables(first, rows, head_dim):
    quarter = head_dim // 4
    half = head_dim // 2
    shape = (rows, head_dim)
    token = first + lax.broadcasted_iota(jnp.int32, shape, 0)
    lane = lax.broadcasted_iota(jnp.int32, shape, 1)
    pair = lane % half
    index = (pair % quarter).astype(F32)
    place = jnp.where(pair < quarter, token // GRID_W, token % GRID_W).astype(F32)
    angle = place * jnp.exp(index * (-math.log(rope_base) / quarter))
    sine = jnp.sin(angle)
    return jnp.cos(angle), jnp.where(lane < half, -sine, sine)


def head_norm(values, gain_row):
    mean = jnp.mean(values * values, axis=-1, keepdims=True)
    return values * lax.rsqrt(mean + norm_eps) * gain_row


def rotate(values, cosine, sine):
    half = values.shape[-1] // 2
    swapped = jnp.concatenate([values[:, half:], values[:, :half]], axis=1)
    return values * cosine + swapped * sine


def kernel(
    sizes,
    condition, code, gain_ref, q_gain, k_gain, bias_ref,
    latent, context, shift_w, scale_w, gate_w, wq, wk, wv, wo,
    out,
    modw, lat, ctx, wq_v, wkv, wbuf,
    vec_z, vec_t, normed, kvbuf, q_s, m_s, acc, att, mixed, cos_s, sin_s, inv_s, out_v,
    local, out_sem,
    z_send, z_recv, t_send, t_recv, kv_send, kv_recv,
    w_send, w_recv, f_send, f_recv, a_send, a_recv,
):
    n_sp, n_tp, n_dp = sizes
    sp, tp, dp = lax.axis_index("sp"), lax.axis_index("tp"), lax.axis_index("dp")
    rows, crows = lat.shape[0], ctx.shape[0]
    hd = wk.shape[0]
    qcols = wq_v.shape[1]
    heads = qcols // hd
    width = lat.shape[1]
    cols = width // n_tp
    dots = functools.partial(jnp.dot, preferred_element_type=F32)

    copies = {}
    for number, (name, src, dst) in enumerate((
        ("m0", shift_w, modw.at[0]), ("m1", scale_w, modw.at[1]), ("m2", gate_w, modw.at[2]),
        ("wk", wk, wkv.at[:hd]), ("wv", wv, wkv.at[hd:]), ("ctx", context.at[0], ctx), ("lat", latent.at[0], lat),
        ("wq", wq, wq_v), ("wo", wo, wbuf.at[tp]),
    )):
        copies[name] = pltpu.make_async_copy(src, dst, local.at[number])
        copies[name].start()

    barrier = pltpu.get_barrier_semaphore()
    for d in range(1, n_sp):
        pl.semaphore_signal(barrier, inc=1, device_id={"sp": (sp + d) % n_sp}, device_id_type=pl.DeviceIdType.MESH)
    for d in range(1, n_tp):
        pl.semaphore_signal(barrier, inc=1, device_id={"tp": tp ^ d}, device_id_type=pl.DeviceIdType.MESH)
    for d in range(1, n_dp):
        pl.semaphore_signal(barrier, inc=1, device_id={"dp": (dp + d) % n_dp}, device_id_type=pl.DeviceIdType.MESH)

    def remote(src, dst, s, r, **where):
        return pltpu.make_async_remote_copy(
            src_ref=src, dst_ref=dst, send_sem=s, recv_sem=r,
            device_id=where, device_id_type=pl.DeviceIdType.MESH)

    row8 = lax.broadcasted_iota(jnp.int32, (8, condition.shape[1]), 0)
    own_code = condition[...].astype(F32)
    shared_code = code[...].astype(F32)[None]
    both = jnp.where(row8 == 0, own_code, jnp.where(row8 == 1, shared_code, 0.0))
    both = (both / (1.0 + jnp.exp(-both))).astype(BF16)
    pieces = []
    for k in range(3):
        copies[f"m{k}"].wait()
        pieces.append(dots(both, modw[k])[:2])
    vec_z[sp] = jnp.concatenate(pieces + [jnp.zeros_like(pieces[0])], axis=0)

    pl.semaphore_wait(barrier, n_sp + n_tp + n_dp - 3)
    z_copies = []
    for d in range(1, n_sp):
        copy = remote(vec_z.at[sp], vec_z.at[sp], z_send.at[d], z_recv.at[d], sp=(sp + d) % n_sp)
        copy.start()
        z_copies.append(copy)

    share = wo.shape[0] // n_dp
    piece = share // 2

    def span(core, part):
        return pl.ds(core * share + part * piece, piece)

    near = [d for d in (1, 2) if d < n_tp]
    waiting = []

    def send_weights(part):
        for d in near:
            copy = remote(wo.at[span(dp, part)], wbuf.at[tp, span(dp, part)],
                          w_send.at[d, part], w_recv.at[d, part], tp=tp ^ d)
            copy.start()
            waiting.append(copy)

    def got_weights(d, part):
        ref = wbuf.at[tp ^ d, span(dp, part)]
        remote(ref, ref, w_send.at[d, part], w_recv.at[d, part], tp=tp ^ d).wait_recv()
        if n_tp == 4 and (d, part) in ((2, 0), (1, 1)):
            copy = remote(ref, ref, w_send.at[3, part], w_recv.at[3, part], tp=tp ^ (3 - d))
            copy.start()
            waiting.append(copy)
        for e in range(1, n_dp):
            copy = remote(ref, ref, f_send.at[d, part, e], f_recv.at[d, part, e], dp=(dp + e) % n_dp)
            copy.start()
            waiting.append(copy)

    send_weights(0)

    cosine, sine = tables(sp * rows, rows, hd)
    cos_s[...] = cosine
    sin_s[...] = sine
    copies["ctx"].wait()
    floats = ctx[...].astype(F32)
    inv_c = lax.rsqrt(jnp.mean(floats * floats, axis=-1, keepdims=True) + norm_eps)
    copies["lat"].wait()
    floats = lat[...].astype(F32)
    inv_s[...] = lax.rsqrt(jnp.mean(floats * floats, axis=-1, keepdims=True) + norm_eps)

    for copy in z_copies:
        copy.wait()
    total = vec_z[0]
    for k in range(1, n_sp):
        total = total + vec_z[k]
    vec_t[tp] = total
    for d in range(1, n_tp):
        copy = remote(vec_t.at[tp], vec_t.at[tp], t_send.at[d], t_recv.at[d], tp=tp ^ d)
        copy.start()
        waiting.append(copy)
    send_weights(1)
    for d in range(1, n_tp):
        remote(vec_t.at[tp ^ d], vec_t.at[tp ^ d], t_send.at[d], t_recv.at[d], tp=tp ^ d).wait_recv()

    def modulate(tokens, inverse, which):
        for t in range(n_tp):
            part = slice(t * cols, (t + 1) * cols)
            factor = gain_ref[:, part] * (1.0 + vec_t[t, 2 + which:3 + which, :])
            shift = vec_t[t, which:which + 1, :]
            normed[:tokens.shape[0], part] = (tokens[:, part].astype(F32) * inverse * factor + shift).astype(BF16)

    lanes = 2 * hd

    def kv_copy(block, target, way, part):
        area = pl.ds(0, crows) if part == 0 else pl.ds(crows, rows)
        ref = kvbuf.at[block, area]
        return remote(ref, ref, kv_send.at[way, part, block], kv_recv.at[part, block], sp=target)

    def send_own(part):
        @pl.when(sp + 1 < n_sp)
        def _():
            kv_copy(sp, sp + 1, 0, part).start()

        @pl.when(sp > 0)
        def _():
            kv_copy(sp, sp - 1, 1, part).start()

    dims = (((1,), (1,)), ((), ()))
    modulate(ctx, inv_c, 1)
    copies["wk"].wait()
    copies["wv"].wait()
    kv = lax.dot_general(normed[:crows], wkv[...], dims, preferred_element_type=F32)
    kvbuf[sp, :crows] = jnp.concatenate([head_norm(kv[:, :hd], k_gain[...]), kv[:, hd:]], axis=1).astype(BF16)
    send_own(0)

    modulate(lat, inv_s[...], 0)
    kv = lax.dot_general(normed[:rows], wkv[...], dims, preferred_element_type=F32)
    keys = rotate(head_norm(kv[:, :hd], k_gain[...]), cos_s[...], sin_s[...])
    kvbuf[sp, crows:] = jnp.concatenate([keys, kv[:, hd:]], axis=1).astype(BF16)
    send_own(1)

    copies["wq"].wait()
    queries = dots(normed[:rows], wq_v[...])
    for h in range(heads):
        one = rotate(head_norm(queries[:, h * hd:(h + 1) * hd], q_gain[...]), cos_s[...], sin_s[...])
        q_s[h] = (one * hd ** -0.5).astype(BF16)
    m_s[...] = jnp.full_like(m_s, LOW)
    acc[...] = jnp.zeros_like(acc)

    for d in near:
        got_weights(d, 0)

    def absorb(block):
        @pl.loop(0, heads, unroll=2)
        def _(h):
            bias = bias_ref[h]
            query = q_s[h]
            s_c = lax.dot_general(query, kvbuf[block, :crows, :hd], dims, preferred_element_type=F32)
            s_l = lax.dot_general(query, kvbuf[block, crows:, :hd], dims, preferred_element_type=F32)
            old = m_s[h]
            new = jnp.maximum(old, jnp.maximum(
                s_c.max(axis=1, keepdims=True) + bias, s_l.max(axis=1, keepdims=True)))
            m_s[h] = new
            p_c = jnp.exp(s_c - (new - bias)).astype(BF16)
            p_l = jnp.exp(s_l - new).astype(BF16)

            def values(pairs):
                lane = lax.broadcasted_iota(jnp.int32, pairs.shape, 1)
                return jnp.where(lane < hd, jnp.ones_like(pairs), pairs)

            acc[h] = (acc[h] * jnp.exp(old - new)
                      + dots(p_c, values(kvbuf[block, :crows]))
                      + dots(p_l, values(kvbuf[block, crows:])))

    absorb(sp)

    def forward(s):
        for part in range(2):
            @pl.when(sp - s >= 0)
            def _():
                kv_copy(sp - s, sp, 0, part).wait_recv()

                @pl.when(sp + 1 < n_sp)
                def _():
                    kv_copy(sp - s, sp + 1, 0, part).start()

            @pl.when(sp + s < n_sp)
            def _():
                kv_copy(sp + s, sp, 1, part).wait_recv()

                @pl.when(sp > 0)
                def _():
                    kv_copy(sp + s, sp - 1, 1, part).start()

    def absorb_both(s):
        @pl.when(sp - s >= 0)
        def _():
            absorb(sp - s)

        @pl.when(sp + s < n_sp)
        def _():
            absorb(sp + s)

    if n_sp > 1:
        forward(1)
    for d in near:
        got_weights(d, 1)
    if n_sp > 1:
        absorb_both(1)

    @pl.loop(2, n_sp)
    def _(s):
        forward(s)
        absorb_both(s)

    if n_tp == 4:
        for part in range(2):
            got_weights(3, part)

    for g in range(heads // 2):
        pair = []
        for h in (2 * g, 2 * g + 1):
            whole = acc[h]
            pair.append(whole[:, hd:] / whole[:, :hd])
        att[tp, g] = jnp.concatenate(pair, axis=1).astype(BF16)
        for d in range(1, n_tp):
            copy = remote(att.at[tp, g], att.at[tp, g], a_send.at[d, g], a_recv.at[d, g], tp=tp ^ d)
            copy.start()
            waiting.append(copy)

    copies["wo"].wait()
    step = cols

    def project(group):
        left = jnp.concatenate([att[group, g] for g in range(heads // 2)], axis=1)
        return lambda part: dots(left, wbuf[group, :, part]).astype(BF16).astype(F32)

    def arrive(d):
        for core in range(1, n_dp):
            source = (dp + n_dp - core) % n_dp
            for part in range(2):
                ref = wbuf.at[tp ^ d, span(source, part)]
                remote(ref, ref, f_send.at[d, part, core], f_recv.at[d, part, core], dp=source).wait_recv()
        for g in range(heads // 2):
            ref = att.at[tp ^ d, g]
            remote(ref, ref, a_send.at[d, g], a_recv.at[d, g], tp=tp ^ d).wait_recv()
        return project(tp ^ d)

    backs = []
    for d in range(n_tp):
        term = project(tp) if d == 0 else arrive(d)
        for t in range(n_tp):
            part = slice(t * step, (t + 1) * step)
            value = term(part)
            if d > 0:
                value = mixed[:, part] + value
            if d < n_tp - 1:
                mixed[:, part] = value
            else:
                gate = vec_t[t, 4:5, :]
                out_v[:, part] = (lat[:, part].astype(F32) + gate * value).astype(BF16)
                back = pltpu.make_async_copy(out_v.at[:, part], out.at[0, :, part], out_sem.at[t])
                back.start()
                backs.append(back)

    for copy in waiting:
        copy.wait_send()

    @pl.loop(0, n_sp)
    def _(b):
        for part in range(2):
            @pl.when((b <= sp) & (sp + 1 < n_sp))
            def _():
                kv_copy(b, sp, 0, part).wait_send()

            @pl.when((b >= sp) & (sp > 0))
            def _():
                kv_copy(b, sp, 1, part).wait_send()
    for back in backs:
        back.wait()


def on_device(
    sizes, latent, condition, context, context_code, shift_weight, scale_weight, gate_weight,
    norm_gain, query_weight, key_weight, value_weight, output_weight, query_gain, key_gain,
    context_bias,
):
    n_sp, n_tp, n_dp = sizes
    rows, width = latent.shape[1:]
    crows = context.shape[1]
    hd = query_gain.shape[0]
    qcols = query_weight.shape[1]
    heads = qcols // hd
    deep, cols = shift_weight.shape
    vmem = pl.BlockSpec(memory_space=pltpu.VMEM)
    smem = pl.BlockSpec(memory_space=pltpu.SMEM)
    hbm = pl.BlockSpec(memory_space=pl.ANY)
    dma = pltpu.SemaphoreType.DMA
    most = max(rows, crows)
    scratch = [
        pltpu.VMEM((3, deep, cols), BF16),
        pltpu.VMEM((rows, width), BF16),
        pltpu.VMEM((crows, width), BF16),
        pltpu.VMEM((width, qcols), BF16),
        pltpu.VMEM((2 * hd, width), BF16),
        pltpu.VMEM((n_tp,) + output_weight.shape, BF16),
        pltpu.VMEM((n_sp, 8, cols), F32),
        pltpu.VMEM((n_tp, 8, cols), F32),
        pltpu.VMEM((most, width), BF16),
        pltpu.VMEM((n_sp, crows + rows, 2 * hd), BF16),
        pltpu.VMEM((heads, rows, hd), BF16),
        pltpu.VMEM((heads, rows, 1), F32),
        pltpu.VMEM((heads, rows, 2 * hd), F32),
        pltpu.VMEM((n_tp, heads // 2, rows, 2 * hd), BF16),
        pltpu.VMEM((rows, width), F32),
        pltpu.VMEM((rows, hd), F32),
        pltpu.VMEM((rows, hd), F32),
        pltpu.VMEM((rows, 1), F32),
        pltpu.VMEM((rows, width), BF16),
        dma((9,)), dma((n_tp,)),
        dma((n_sp,)), dma((n_sp,)), dma((n_tp,)), dma((n_tp,)),
        dma((2, 2, n_sp)), dma((2, n_sp)),
        dma((n_tp, 2)), dma((n_tp, 2)), dma((n_tp, 2, n_dp)), dma((n_tp, 2, n_dp)),
        dma((n_tp, heads // 2)), dma((n_tp, heads // 2)),
    ]
    return pl.pallas_call(
        functools.partial(kernel, sizes),
        out_shape=jax.ShapeDtypeStruct(latent.shape, BF16),
        in_specs=[vmem] * 5 + [smem] + [hbm] * 9,
        out_specs=hbm,
        scratch_shapes=scratch,
        compiler_params=pltpu.CompilerParams(
            collective_id=0, has_side_effects=True, vmem_limit_bytes=60 * 1024 * 1024),
    )(
        condition, context_code, norm_gain[None], query_gain[None], key_gain[None],
        context_bias, latent, context, shift_weight, scale_weight, gate_weight, query_weight,
        key_weight.T, value_weight.T, output_weight,
    )


def solution(mesh):
    sizes = tuple(mesh.shape[axis] for axis in ("sp", "tp", "dp"))
    return jax.shard_map(
        functools.partial(on_device, sizes),
        mesh=mesh,
        in_specs=(
            P("dp", "sp", None),
            P("dp", "sp"),
            P("dp", "sp", None),
            P("sp"),
            P("sp", "tp"),
            P("sp", "tp"),
            P("sp", "tp"),
            P(),
            P(None, "tp"),
            P(None, "tp"),
            P(None, "tp"),
            P("tp", None),
            P(),
            P(),
            P("tp"),
        ),
        out_specs=P("dp", "sp", None),
        check_vma=False,
    )
```
